32 devices in a mesh: ep: 8 (over z, x), tp: 4 (over y, core).
Axes of the slice: x: 2, y: 2, z: 4, core: 2. Of those that a mesh axis runs over, the one named last changes fastest.
Arguments:
- tokens: bfloat16 [8192, 2048], P(('ep', 'tp')), may hold values from -6 to 6
- norm_gain: bfloat16 [2048], replicated, may hold values from 0.099609375 to 1.8984375
- expert_ids: int32 [8192, 2], P(('ep', 'tp')), may hold values from 0 to 7, all different within a row; in each aligned block of 256 rows (0 to 255, 256 to 511, ...) at most 128 rows name the same one
- group_weight: float32 [8192], P(('ep', 'tp')), may hold values from 0.25 to 1
- expert_logit: float32 [8192, 2], P(('ep', 'tp')), may hold values from -4 to 4
- w_gate: bfloat16 [8, 2048, 1024], P('ep', None, 'tp'), may hold values from -0.125 to 0.125
- w_up: bfloat16 [8, 2048, 1024], P('ep', None, 'tp'), may hold values from -0.125 to 0.125
- w_down: bfloat16 [8, 1024, 2048], P('ep', 'tp')
- final_gain: bfloat16 [2048], P('tp'), may hold values from 0.099609375 to 1.8984375
Outputs:
- normed_out: bfloat16 [8192, 2048], P('ep', 'tp')
The draws below stay inside these ranges and needn't reach their ends.
Inputs may be any that keep to these rules, and one draw needn't show every extreme that they name: `expert_ids`: the 2 experts of a token differ. Among the rows of one device (aligned blocks of 256 tokens) no expert is named more than 128 times, a bound that some block reaches.
All inputs are finite; a program needn't handle non-finite values.
Results may differ from the reference program's by a relative error of at most 0.0058.
Values may be sent and summed in bfloat16 or wider, within the bound.
No kernel may reach another device: no remote copies, remote signals or barrier semaphores. Data moves between devices by JAX's collectives and lax.ppermute only.
A program may use at most 128 MiB of HBM per device.

```python
import math
import jax
import jax.numpy as jnp
import numpy as np
from jax import lax

D = 2048
FF = 1024
TOP = 2
TOK_DEV = 256
EXPERTS = 8
CAP = 128
TOKENS = 8192


def draw_w_down(key, part):
    first, second = jax.random.split(key)
    base = jax.random.normal(first, (EXPERTS, FF, D), jnp.float32)
    levels = jnp.array([0.4, 0.9, 1.5, 2.4], jnp.float32)
    shuffled = levels[jax.random.permutation(second, 4)]
    quarter = jnp.arange(D, dtype=jnp.int32) * 4 // D
    column_scale = shuffled[quarter]
    return (base * FF ** (-0.5) * column_scale[None, None, :]).astype(jnp.bfloat16)


def block_levels(stream_key, extent, shards, smallest, largest):
    loudness, own = 1.0, jax.random.fold_in(stream_key, 6)
    for position, blocks in shards:
        heights = jnp.exp(jax.random.uniform(jax.random.fold_in(own, position), (blocks,), jnp.float32, smallest / len(shards), largest / len(shards)))
        loudness = loudness * jnp.repeat(heights, extent[position] // blocks).reshape([-1 if axis == position else 1 for axis in range(len(extent))])
    return loudness


def shared_out(key, own, number, rows, number_of, top, limit, slope):
    ranking = jax.random.permutation(key, number_of)
    packed, common = shares(number_of, rows * top, limit, slope, True), shares(number_of, rows * top, limit, slope, False)
    places = jnp.arange(number_of)

    def named(tallies, rotation):
        used = int((tallies > 0).sum())
        fixed = max(1, used // 4)
        passed = fixed + (places - fixed + rotation * (used - fixed)) % max(1, number_of - fixed)
        return jnp.zeros((number_of,), jnp.int32).at[ranking[jnp.where(places < fixed, places, passed)]].set(jnp.asarray(tallies, jnp.int32))

    tallies = jnp.where(number % 4 == 0, named(packed, number // 4), named(common, number - number // 4 - 1))
    mixed = jax.random.permutation(jax.random.fold_in(own, 3), number_of)
    giver, sink = mixed[0:number_of // 2 * 2:2], mixed[1:number_of // 2 * 2:2]
    slack = jnp.minimum(tallies[giver] - 1, limit - tallies[sink]) // 2
    slack = jnp.where((giver == ranking[0]) | (sink == ranking[0]) | (tallies[sink] == 0), 0, jnp.maximum(slack, 0))
    passed = jax.random.randint(jax.random.fold_in(own, 4), (number_of // 2,), 0, 1 << 20) % (slack + 1)
    tallies = tallies.at[giver].add(-passed).at[sink].add(passed)
    labels = jnp.searchsorted(jnp.cumsum(tallies), jnp.arange(rows * top), side="right").astype(jnp.int32)
    grid = labels.reshape(top, rows).T
    grid = grid[jax.random.permutation(jax.random.fold_in(own, 1), rows)]
    rotation = jax.random.randint(jax.random.fold_in(own, 2), (rows, 1), 0, top)
    return jnp.take_along_axis(grid, (jnp.arange(top)[None, :] + rotation) % top, axis=1)


def shares(count, total, reach, slope, full):
    loads = [(1 << 20) // math.isqrt(standing ** slope) + 1 for standing in range(1, count + 1)]
    largest = reach if full else min(reach, max(-(-total // count), total * loads[0] // sum(loads)))
    least = 1 if total - largest >= count - 1 else 0
    holding, spare = [largest] + [least] * (count - 1), total - largest - least * (count - 1)
    while spare > 0:
        candidates = [i for i in range(1, count) if holding[i] < largest] or [i for i in range(1, count) if holding[i] < reach]
        mass, remaining = sum([loads[i] for i in candidates]), spare
        for i in candidates:
            more = min(reach - holding[i], max(1, remaining * loads[i] // mass), spare)
            holding[i] = holding[i] + more
            spare = spare - more
    return np.array(holding)


def noise(key, dims, deviation, most, cuts=(), held_as=jnp.bfloat16):
    values = jax.random.normal(key, dims, jnp.float32) * deviation
    if len(cuts) > 0:
        values = block_levels(key, dims, cuts, -0.22, 0.18) * values
    return jnp.clip(values, min=-most, max=most).astype(held_as)


def setup_inputs(seed: int = 0) -> dict:
    key_list = jax.random.split(jax.random.key(seed), 10)
    tokens = noise(key_list[0], (TOKENS, D), 1.0, 6.0, ((0, 32),))
    norm_gain = jnp.clip(1.0 + 0.18 * jax.random.normal(key_list[1], (D,), jnp.float32), 0.099609375, 1.8984375).astype(jnp.bfloat16)
    expert_ids_keys = jax.random.split(jax.random.fold_in(key_list[2], 1), TOKENS // TOK_DEV)
    expert_ids_turns = jax.random.permutation(jax.random.fold_in(key_list[2], 3), TOKENS // TOK_DEV)
    expert_ids = jax.vmap(lambda own, number: shared_out(jax.random.fold_in(key_list[2], 2), own, number, TOK_DEV, EXPERTS, TOP, CAP, 2))(expert_ids_keys, expert_ids_turns).reshape((TOKENS, TOP))
    group_weight = jnp.clip(0.25 + 0.75 * jax.random.uniform(key_list[3], (TOKENS,), jnp.float32) ** block_levels(key_list[3], (TOKENS,), ((0, 32),), -0.2, 0.2), 0.25, 1.0)
    expert_logit = noise(key_list[4], (TOKENS, TOP), 1.5, 4.0, ((0, 32),), jnp.float32)
    w_gate = noise(key_list[5], (EXPERTS, D, FF), D ** -0.5, 0.125, ((0, 8), (2, 4)))
    w_up = noise(key_list[6], (EXPERTS, D, FF), D ** -0.5, 0.125, ((0, 8), (2, 4)))
    w_down = draw_w_down(jax.random.fold_in(key_list[9], 71), 0)
    final_gain = jnp.clip(1.0 + 0.18 * jax.random.normal(key_list[8], (D,), jnp.float32), 0.099609375, 1.8984375).astype(jnp.bfloat16)
    return dict(tokens=tokens, norm_gain=norm_gain, expert_ids=expert_ids, group_weight=group_weight, expert_logit=expert_logit, w_gate=w_gate, w_up=w_up, w_down=w_down, final_gain=final_gain)


EPS = 1e-06

def normalize(values, gain):
    return values * lax.rsqrt(lax.optimization_barrier(jnp.mean(values * values, axis=-1, keepdims=True)) + EPS) * gain.astype(jnp.float32)

def reference(tokens, norm_gain, expert_ids, group_weight, expert_logit, w_gate, w_up, w_down, final_gain):
    block_len = 256
    tokens_f = tokens.astype(jnp.float32)
    normed_in = normalize(tokens_f, norm_gain).astype(jnp.bfloat16)
    total_tok, per_token = expert_ids.shape
    experts = w_gate.shape[0]
    assigned = total_tok * per_token
    flat_ids = expert_ids.reshape(assigned).astype(jnp.int32)
    sort_order = jnp.argsort(flat_ids, stable=True).astype(jnp.int32)
    sorted_ids = flat_ids[sort_order]
    counts = jnp.bincount(flat_ids, length=experts).astype(jnp.int32)
    starts = (jnp.cumsum(counts) - counts).astype(jnp.int32)
    padded = (counts + block_len - 1) // block_len * block_len
    ends = jnp.cumsum(padded).astype(jnp.int32)
    pad_starts = (ends - padded).astype(jnp.int32)
    target = (pad_starts[sorted_ids] + jnp.arange(assigned, dtype=jnp.int32) - starts[sorted_ids]).astype(jnp.int32)
    blocks = assigned // block_len + experts + 1
    row_token = jnp.zeros((blocks * block_len,), jnp.int32).at[target].set((sort_order // per_token).astype(jnp.int32))
    block_expert = jnp.minimum(jnp.searchsorted(ends, jnp.arange(blocks, dtype=jnp.int32) * block_len, side='right'), experts - 1).astype(jnp.int32)
    inputs = normed_in[row_token].reshape(blocks, block_len, normed_in.shape[1])

    def expert_block(pair):
        rows, which = pair
        gate = jnp.dot(rows, w_gate[which], preferred_element_type=jnp.float32)
        upper = jnp.dot(rows, w_up[which], preferred_element_type=jnp.float32)
        hidden = (jax.nn.silu(gate) * upper).astype(jnp.bfloat16)
        return jnp.dot(hidden, w_down[which], preferred_element_type=jnp.float32).astype(jnp.bfloat16)
    outputs = lax.map(expert_block, (inputs, block_expert)).reshape(blocks * block_len, normed_in.shape[1])
    where_row = jnp.zeros((assigned,), jnp.int32).at[sort_order].set(target).reshape(total_tok, per_token)
    expert_share = jnp.exp(expert_logit)
    expert_share = expert_share / lax.optimization_barrier(jnp.sum(expert_share, axis=-1, keepdims=True))
    route_weight = group_weight[:, None] * expert_share
    mixture = tokens_f
    for member in range(per_token):
        mixture = mixture + route_weight[:, member:member + 1] * outputs[where_row[:, member]].astype(jnp.float32)
    residual = mixture.astype(jnp.bfloat16).astype(jnp.float32)
    return normalize(residual, final_gain).astype(jnp.bfloat16)
```

```python
import functools

import jax
import jax.numpy as jnp
from jax import lax
from jax.experimental import pallas as pl
from jax.experimental.pallas import tpu as pltpu
from jax.sharding import PartitionSpec as P

D = 2048


EPS = 1e-06
BF16, F32 = jnp.bfloat16, jnp.float32
LEVELS, COLUMNS = 4, 2
TP = 4
ANY = pl.BlockSpec(memory_space=pl.ANY)
SMEM = pl.BlockSpec(memory_space=pltpu.SMEM)
VMEM = pl.BlockSpec(memory_space=pltpu.VMEM)
PARAMS = pltpu.CompilerParams(vmem_limit_bytes=56 * 1024 * 1024)


def flat_plan(
    tokens, norm_gain, expert_ids, group_weight, expert_logit, w_gate, w_up, w_down, final_gain
):
    tok_dev, width = tokens.shape
    per_token = expert_ids.shape[1]
    exp_dev = w_gate.shape[0]
    experts = exp_dev * lax.axis_size("ep")
    capacity = 2 * tok_dev * per_token // experts
    assigned = tok_dev * per_token
    tokens_f = tokens.astype(jnp.float32)
    inverse_in = lax.rsqrt(jnp.mean(tokens_f * tokens_f, axis=-1, keepdims=True) + EPS)
    normed_in = (tokens_f * inverse_in * norm_gain.astype(jnp.float32)).astype(jnp.bfloat16)
    flat_ids = expert_ids.reshape(assigned)
    onehot = (flat_ids[:, None] == jnp.arange(experts, dtype=jnp.int32)[None, :]).astype(jnp.int32)
    before = jnp.cumsum(onehot, axis=0) - onehot
    slot_rank = jnp.sum(before * onehot, axis=1)
    position = slot_rank * experts + flat_ids
    owner_row = (
        jnp.zeros((capacity * experts,), jnp.int32)
        .at[position]
        .set(jnp.arange(assigned, dtype=jnp.int32) // per_token + 1)
    )
    source = normed_in[jnp.maximum(owner_row - 1, 0)]
    outgoing = jnp.where((owner_row > 0)[:, None], source, jnp.zeros_like(source)).reshape(
        capacity, experts, width
    )
    down_whole = lax.all_gather(w_down, "tp", axis=1, tiled=True)
    gate_whole, up_whole = (
        lax.all_gather(w_gate, "tp", axis=2, tiled=True),
        lax.all_gather(w_up, "tp", axis=2, tiled=True),
    )
    incoming = lax.all_to_all(outgoing, "ep", split_axis=1, concat_axis=1, tiled=True)
    item_count = incoming.shape[0]
    senders = incoming.shape[1] // exp_dev
    arranged = incoming.reshape(item_count, senders, exp_dev, width)
    routed = arranged[:, :, 0, :].reshape(item_count * senders, width)
    gate_full = jnp.dot(routed, gate_whole[0], preferred_element_type=jnp.float32)
    up_full = jnp.dot(routed, up_whole[0], preferred_element_type=jnp.float32)
    hidden = (jax.nn.silu(gate_full) * up_full).astype(jnp.bfloat16)
    product = jnp.dot(hidden, down_whole[0], preferred_element_type=jnp.float32).astype(
        jnp.bfloat16
    )
    results = [product.reshape(item_count, senders, width)]
    answer = jnp.stack(results, axis=2).reshape(item_count, senders * exp_dev, width)
    arrived = lax.all_to_all(answer, "ep", split_axis=1, concat_axis=1, tiled=True)
    picked = arrived.reshape(capacity * experts, width)[position].reshape(tok_dev, per_token, width)
    expert_share = jnp.exp(expert_logit)
    expert_share = expert_share / jnp.sum(expert_share, axis=-1, keepdims=True)
    route_weight = group_weight[:, None] * expert_share
    mixture = tokens_f + jnp.sum(route_weight[:, :, None] * picked.astype(jnp.float32), axis=1)
    residual = mixture.astype(jnp.bfloat16)
    sliced = lax.all_to_all(residual, "tp", split_axis=1, concat_axis=0, tiled=True).astype(
        jnp.float32
    )
    squares = lax.psum(jnp.sum(sliced * sliced, axis=-1), "tp")
    inverse_out = lax.rsqrt(squares / D + EPS)
    return (sliced * inverse_out[:, None] * final_gain.astype(jnp.float32)).astype(jnp.bfloat16)


def expert_rows(meta, expert, slots, weighted):
    tok = meta.shape[1]
    first, second = meta[0:1, :] == expert, meta[1:2, :] == expert
    member = jnp.where(first | second, 1.0, 0.0).astype(F32)
    earlier = (
        lax.broadcasted_iota(jnp.int32, (tok, tok), 0)
        < lax.broadcasted_iota(jnp.int32, (tok, tok), 1)
    ).astype(F32)
    rank = jnp.dot(
        jnp.broadcast_to(member, (8, tok)).astype(BF16),
        earlier.astype(BF16),
        preferred_element_type=F32,
    )[0:1, :]
    key = jnp.where(member > 0.0, rank, -1.0)
    here = key == lax.broadcasted_iota(jnp.int32, (slots, tok), 0).astype(F32)
    if not weighted:
        return jnp.where(here, 1.0, 0.0).astype(F32)
    weight = jnp.where(first, meta[2:3, :], jnp.where(second, meta[3:4, :], 0.0))
    return jnp.where(here, weight, 0.0)


def pick_body(pos, table, gain, *refs, count, slots):
    blocks = refs[:count]
    own_out, side_out, block, sem = refs[count:]
    for number in range(count):

        @pl.when(pos[0] == number)
        def _():
            copy = pltpu.make_async_copy(blocks[number], block, sem)
            copy.start()
            copy.wait()

    meta = table[pos[1]]
    width = block.shape[1]
    step = 32

    def norm(index, carry):
        rows = pl.ds(pl.multiple_of(index * step, step), step)
        values = block[rows, :].astype(F32)
        inverse = lax.rsqrt(jnp.mean(values * values, axis=-1, keepdims=True) + EPS)
        block[rows, :] = (values * inverse * gain[...].astype(F32)).astype(BF16)
        return carry

    lax.fori_loop(0, block.shape[0] // step, norm, 0)
    for expert, out in ((pos[2], own_out), (pos[3], side_out)):
        chosen = expert_rows(meta, expert.astype(F32), slots, False).astype(BF16)
        for start in range(0, width, 512):
            out[:, start : start + 512] = jnp.dot(
                chosen, block[:, start : start + 512], preferred_element_type=F32
            ).astype(BF16)


def pick(pos, table, gain, blocks, slots):
    rows = jax.ShapeDtypeStruct((slots, blocks[0].shape[1]), BF16)
    return pl.pallas_call(
        functools.partial(pick_body, count=len(blocks), slots=slots),
        in_specs=[SMEM, VMEM, VMEM] + [ANY] * len(blocks),
        out_specs=[VMEM, VMEM],
        out_shape=[rows, rows],
        scratch_shapes=[pltpu.VMEM(blocks[0].shape, BF16), pltpu.SemaphoreType.DMA],
        compiler_params=PARAMS,
        name="pick",
    )(pos, table, gain, *blocks)


def experts_body(*refs, count, pieces):
    inputs = refs[:count]
    gates = refs[count : count + pieces]
    ups = refs[count + pieces : count + 2 * pieces]
    downs = refs[count + 2 * pieces : count + 3 * pieces]
    outs = refs[count + 3 * pieces : 2 * count + 3 * pieces]
    rows, gate, up, down, hidden, row_sem, weight_sem = refs[2 * count + 3 * pieces :]
    part = gate.shape[2]
    slots = inputs[0].shape[0]
    width = rows.shape[1]
    row_copies = [
        pltpu.make_async_copy(ref, rows.at[pl.ds(n * slots, slots)], row_sem.at[n])
        for n, ref in enumerate(inputs)
    ]
    copies = []
    for n in range(pieces):
        copies.append(pltpu.make_async_copy(gates[n].at[0], gate.at[n], weight_sem.at[n, 0]))
        copies.append(pltpu.make_async_copy(ups[n].at[0], up.at[n], weight_sem.at[n, 1]))
    for n in range(pieces):
        copies.append(
            pltpu.make_async_copy(
                downs[n].at[0], down.at[pl.ds(n * part, part)], weight_sem.at[n, 2]
            )
        )
    for copy in row_copies + copies:
        copy.start()
    for copy in row_copies:
        copy.wait()
    for n in range(pieces):
        copies[2 * n].wait()
        copies[2 * n + 1].wait()
        gated = jnp.dot(rows[...], gate[n], preferred_element_type=F32)
        upper = jnp.dot(rows[...], up[n], preferred_element_type=F32)
        hidden[:, n * part : (n + 1) * part] = (
            gated / (1.0 + jnp.exp(-gated)) * upper
        ).astype(BF16)
    for n in range(pieces):
        copies[2 * pieces + n].wait()
    for start in range(0, width, 512):
        product = jnp.dot(
            hidden[...], down[:, start : start + 512], preferred_element_type=F32
        ).astype(BF16)
        for n, out in enumerate(outs):
            out[:, start : start + 512] = product[n * slots : (n + 1) * slots]


def experts(inputs, gates, ups, downs):
    count, pieces = len(inputs), len(gates)
    slots, width = inputs[0].shape
    part = gates[0].shape[2]
    total = count * slots
    return pl.pallas_call(
        functools.partial(experts_body, count=count, pieces=pieces),
        in_specs=[ANY] * (count + 3 * pieces),
        out_specs=[VMEM] * count,
        out_shape=[jax.ShapeDtypeStruct((slots, width), BF16)] * count,
        scratch_shapes=[
            pltpu.VMEM((total, width), BF16),
            pltpu.VMEM((pieces, width, part), BF16),
            pltpu.VMEM((pieces, width, part), BF16),
            pltpu.VMEM((pieces * part, width), BF16),
            pltpu.VMEM((total, pieces * part), BF16),
            pltpu.SemaphoreType.DMA((count,)),
            pltpu.SemaphoreType.DMA((pieces, 3)),
        ],
        compiler_params=PARAMS,
        cost_estimate=pl.CostEstimate(
            flops=6 * total * width * pieces * part,
            bytes_accessed=6 * width * pieces * part + 4 * total * width,
            transcendentals=total * pieces * part,
        ),
        name="experts",
    )(*inputs, *gates, *ups, *downs)


def mix_body(pos, table, own, side, *refs):
    out = refs[-1]
    slots, width = own.shape
    meta = table[pos[1]]
    parts = []
    for expert, rows in ((pos[2], own), (pos[3], side)):
        weights = expert_rows(meta, expert.astype(F32), slots, True).T
        high = weights.astype(BF16)
        low = (weights - high.astype(F32)).astype(BF16)
        parts.append((high, low, rows))
    for start in range(0, width, 512):
        total = 0.0
        for high, low, rows in parts:
            values = rows[:, start : start + 512]
            total = total + jnp.dot(high, values, preferred_element_type=F32)
            total = total + jnp.dot(low, values, preferred_element_type=F32)
        for more in refs[:-1]:
            total = total + more[:, start : start + 512].astype(F32)
        out[:, start : start + 512] = total.astype(out.dtype)


def mix(pos, table, own, side, more, dtype):
    tok = table.shape[2]
    return pl.pallas_call(
        mix_body,
        in_specs=[SMEM] + [VMEM] * (3 + len(more)),
        out_specs=VMEM,
        out_shape=jax.ShapeDtypeStruct((tok, own.shape[1]), dtype),
        compiler_params=PARAMS,
        name="mix",
    )(pos, table, own, side, *more)


def close_body(base, first, second, gain, out):
    step = 32

    def norm(index, carry):
        rows = pl.ds(pl.multiple_of(index * step, step), step)
        values = base[rows, :] + first[rows, :].astype(F32) + second[rows, :].astype(F32)
        values = values.astype(BF16).astype(F32)
        inverse = lax.rsqrt(jnp.mean(values * values, axis=-1, keepdims=True) + EPS)
        out[rows, :] = (values * inverse * gain[...].astype(F32)).astype(BF16)
        return carry

    lax.fori_loop(0, out.shape[0] // step, norm, 0)


def close(base, first, second, gain):
    return pl.pallas_call(
        close_body,
        in_specs=[VMEM] * 4,
        out_specs=VMEM,
        out_shape=jax.ShapeDtypeStruct(base.shape, BF16),
        compiler_params=PARAMS,
        name="close",
    )(base, first, second, gain)


def hops(moves):
    return [
        (a * COLUMNS + col, b * COLUMNS + col) for a, b in moves for col in range(COLUMNS)
    ]


def staged_plan(
    tokens, norm_gain, expert_ids, group_weight, expert_logit, w_gate, w_up, w_down, final_gain
):
    tok_dev, width = tokens.shape
    per_token = expert_ids.shape[1]
    ranks = lax.axis_size("ep")
    slots = 2 * tok_dev * per_token // ranks
    me = lax.axis_index("ep")
    level = me // COLUMNS
    lower = level < LEVELS // 2

    def line(value, *moves):
        return lax.ppermute(value, "ep", hops(moves))

    def across(value):
        return lax.ppermute(value, "ep", [(n, n ^ 1) for n in range(ranks)])

    def twin(value, flip):
        return lax.ppermute(value, "tp", [(n, n ^ flip) for n in range(TP)])

    expert_share = jnp.exp(expert_logit)
    expert_share = expert_share / jnp.sum(expert_share, axis=-1, keepdims=True)
    route_weight = group_weight[:, None] * expert_share
    meta = jnp.concatenate(
        [
            expert_ids.T.astype(F32),
            route_weight.T,
            jnp.zeros((8 - 2 * per_token, tok_dev), F32),
        ]
    )
    table = lax.all_to_all(
        jnp.broadcast_to(meta[None], (ranks,) + meta.shape), "ep", 0, 0, tiled=True
    )
    gain_out = lax.all_to_all(
        jnp.broadcast_to(final_gain[None], (TP,) + final_gain.shape), "tp", 0, 0, tiled=True
    ).reshape(1, width)
    gain_in = norm_gain.reshape(1, width)

    up1 = line(tokens, (0, 1), (1, 2), (2, 3))
    down1 = line(tokens, (3, 2), (2, 1), (1, 0))
    weights = [[w, None, twin(w, 2), None] for w in (w_gate, w_up, w_down)]
    for pieces in weights:
        pieces[1] = twin(pieces[0], 1)
        pieces[3] = twin(pieces[2], 1)
    up2 = line(up1, (1, 2), (2, 3))
    down2 = line(down1, (2, 1), (1, 0))
    up3 = line(up2, (2, 3))
    down3 = line(down2, (1, 0))

    def slot(which, source):
        source = source * COLUMNS + me % COLUMNS
        return jnp.stack([which, source, me, me ^ 1]).astype(jnp.int32)

    far = 1 - lower.astype(jnp.int32)
    sign = 1 - 2 * far
    places = [
        slot(0 * me, level),
        slot(far, level + sign),
        slot(far, level + 2 * sign),
        slot(level, (LEVELS - 1) * (1 - level % 2)),
    ]
    blocks = [(tokens,), (down1, up1), (down2, up2), (down3, up1, down1, up3)]
    picked = [pick(p, table, gain_in, b, slots) for p, b in zip(places, blocks)]
    rows = [(own, across(side)) for own, side in picked]
    near = experts([r for pair in rows[:3] for r in pair], *weights)
    last = experts(list(rows[3]), *weights)
    done = [(near[0], near[1]), (near[2], near[3]), (near[4], near[5]), (last[0], last[1])]
    back = [(own, across(side)) for own, side in reversed(done)][::-1]

    sums3 = mix(places[3], table, *back[3], (), BF16)
    got1 = line(sums3, (0, 1), (3, 2))
    sums2 = mix(places[2], table, *back[2], (got1,), BF16)
    got_up, got_down = line(sums2, (0, 1), (1, 2)), line(sums2, (3, 2), (2, 1))
    sums1 = mix(places[1], table, *back[1], (), BF16)
    base = mix(places[0], table, *back[0], (tokens,), F32)

    def join(level_of_last, got):
        mine = jnp.where(level == level_of_last, sums3, sums1)
        return (mine.astype(F32) + got.astype(F32)).astype(BF16)

    first = line(join(2, got_up), (0, 1), (1, 2), (2, 3))
    second = line(join(1, got_down), (3, 2), (2, 1), (1, 0))
    normed = close(base, first, second, gain_out)
    return lax.all_to_all(normed, "tp", split_axis=1, concat_axis=0, tiled=True)


def solution(mesh):
    placed = (
        P(("ep", "tp"), None),
        P(),
        P(("ep", "tp"), None),
        P(("ep", "tp")),
        P(("ep", "tp"), None),
        P("ep", None, "tp"),
        P("ep", None, "tp"),
        P("ep", "tp", None),
        P("tp"),
    )
    line = mesh.shape["ep"] == LEVELS * COLUMNS and mesh.shape["tp"] == TP
    return jax.shard_map(
        staged_plan if line else flat_plan,
        mesh=mesh,
        in_specs=placed,
        out_specs=P("ep", "tp"),
        check_vma=False,
    )
```
